32 devices in a mesh: sp: 16 (over z, y, core), tp: 2 (over x).
Axes of the slice: x: 2, y: 2, z: 4, core: 2. Of those that a mesh axis runs over, the one named last changes fastest.
Arguments:
- query_content: bfloat16 [3072, 1024], P('sp'), may hold values from -6 to 6
- query_rotary: bfloat16 [3072, 512], P('sp'), may hold values from -8 to 8
- latents: bfloat16 [3072, 256], P(('sp', 'tp')), may hold values from -6 to 6
- key_rotary: bfloat16 [3072, 64], P(('sp', 'tp')), may hold values from -8 to 8
- latent_gain: float32 [256], replicated, may hold values from 0.1 to 1.9
- key_up: bfloat16 [256, 1024], P(None, 'tp'), may hold values from -0.375 to 0.375
- value_up: bfloat16 [256, 1024], P(None, 'tp'), may hold values from -0.375 to 0.375
- out_proj: bfloat16 [1024, 2048], P(None, 'tp'), may hold values from -2 to 2
- residual: bfloat16 [3072, 2048], P('sp', 'tp'), may hold values from -6 to 6
- mixer_gain: float32 [2048], replicated, may hold values from 0.1 to 1.9
- gate_proj: bfloat16 [2048, 5632], P('sp', 'tp'), may hold values from -0.125 to 0.125
- up_proj: bfloat16 [2048, 5632], P('sp', 'tp'), may hold values from -0.125 to 0.125
- down_proj: bfloat16 [5632, 2048], P('tp', 'sp'), may hold values from -0.078125 to 0.078125
Outputs:
- layer_out: bfloat16 [3072, 2048], P('sp', 'tp')
The draws below stay inside these ranges and needn't reach their ends.
All inputs are finite; a program needn't handle non-finite values.
Results may differ from the reference program's by a relative error of at most 0.011.
Values may be sent and summed in bfloat16 or wider, within the bound.
A program may use at most 128 MiB of HBM per device.

```python
import math
import jax
import jax.numpy as jnp
from jax import lax

D = 2048
H = 8
DN = 128
DR = 64
DV = 128
KVR = 256
FF = 5632
SPAN = 64
TOK = 192
SEQ = 3072
N_SP = 16
N_TP = 2


def draw_query_rotary(key, part):
    base = jax.random.normal(jax.random.fold_in(key, 14), (SEQ, H * DR), jnp.float32)
    return jnp.clip(base, -6.0, 6.0).astype(jnp.bfloat16)


def draw_key_rotary(key, part):
    base = jax.random.normal(jax.random.fold_in(key, 15), (SEQ, DR), jnp.float32)
    return jnp.clip(base, -6.0, 6.0).astype(jnp.bfloat16)


def shard_levels(own_key, dims, shards, least, high):
    level, own = 1.0, jax.random.fold_in(own_key, 6)
    for position, parts in shards:
        heights = jnp.exp(jax.random.uniform(jax.random.fold_in(own, position), (parts,), jnp.float32, least / len(shards), high / len(shards)))
        level = level * jnp.repeat(heights, dims[position] // parts).reshape([-1 if axis == position else 1 for axis in range(len(dims))])
    return level


def scatter_about(stream_key, shape, deviation, limit, pieces=(), kind=jnp.bfloat16):
    result = deviation * jax.random.normal(stream_key, shape, jnp.float32)
    if pieces:
        result = result * shard_levels(stream_key, shape, pieces, -0.22, 0.18)
    return jnp.clip(result, -limit, limit).astype(kind)


def setup_inputs(seed: int = 0) -> dict:
    key_of = jax.random.split(jax.random.key(seed), 14)
    query_content = scatter_about(key_of[0], (SEQ, H * DN), 1.0, 6.0, ((0, 16),))
    query_rotary = draw_query_rotary(jax.random.fold_in(key_of[13], 71), 0)
    latents = scatter_about(key_of[2], (SEQ, KVR), 1.0, 6.0, ((0, 32),))
    key_rotary = draw_key_rotary(jax.random.fold_in(key_of[13], 71), 0)
    latent_gain = jnp.clip(1.0 + 0.18 * jax.random.normal(key_of[4], (KVR,), jnp.float32), 0.1, 1.9)
    key_up = scatter_about(key_of[5], (KVR, H * DN), KVR ** -0.5, 0.375, ((1, 2),))
    value_up = scatter_about(key_of[6], (KVR, H * DV), KVR ** -0.5, 0.375, ((1, 2),))
    out_proj = scatter_about(key_of[7], (H * DV, D), (H * DV // 128) ** -0.5, 2.0, ((1, 2),))
    residual = scatter_about(key_of[8], (SEQ, D), 1.0, 6.0, ((0, 16), (1, 2)))
    mixer_gain = jnp.clip(1.0 + 0.18 * jax.random.normal(key_of[9], (D,), jnp.float32), 0.1, 1.9)
    gate_proj = scatter_about(key_of[10], (D, FF), D ** -0.5, 0.125, ((0, 16), (1, 2)))
    up_proj = scatter_about(key_of[11], (D, FF), D ** -0.5, 0.125, ((0, 16), (1, 2)))
    down_proj = scatter_about(key_of[12], (FF, D), FF ** -0.5, 0.078125, ((0, 2), (1, 16)))
    return {"query_content": query_content, "query_rotary": query_rotary, "latents": latents, "key_rotary": key_rotary, "latent_gain": latent_gain, "key_up": key_up, "value_up": value_up, "out_proj": out_proj, "residual": residual, "mixer_gain": mixer_gain, "gate_proj": gate_proj, "up_proj": up_proj, "down_proj": down_proj}


epsilon = 1e-06
masked_score = -1e+30

def norm_round(inputs, scales):
    widened = inputs.astype(jnp.float32)
    factor = lax.rsqrt(lax.optimization_barrier(jnp.mean(widened * widened, axis=-1, keepdims=True)) + epsilon)
    return (widened * factor * scales.astype(jnp.float32)).astype(jnp.bfloat16)

def rotate(inputs, places):
    dimension = inputs.shape[-1]
    middle = dimension // 2
    inverse = 10000.0 ** (-jnp.arange(0, dimension, 2, dtype=jnp.float32) / dimension)
    angles = places.astype(jnp.float32)[:, None, None] * inverse[None, None, :]
    cosine_table = jnp.cos(angles)
    sine_table = jnp.sin(angles)
    widened = inputs.astype(jnp.float32)
    first_half = widened[..., :middle]
    second_half = widened[..., middle:]
    return jnp.concatenate([first_half * cosine_table - second_half * sine_table, second_half * cosine_table + first_half * sine_table], axis=-1).astype(jnp.bfloat16)

def reference(query_content, query_rotary, latents, key_rotary, latent_gain, key_up, value_up, out_proj, residual, mixer_gain, gate_proj, up_proj, down_proj):
    per_device = TOK // N_TP
    normed = norm_round(latents, latent_gain)
    key_content = jnp.dot(normed, key_up, preferred_element_type=jnp.float32).astype(jnp.bfloat16)
    values = jnp.dot(normed, value_up, preferred_element_type=jnp.float32).astype(jnp.bfloat16)
    places = jnp.arange(SEQ, dtype=jnp.int32)
    key_turned = rotate(key_rotary[:, None, :], places)[:, 0, :]
    query_turned = rotate(query_rotary.reshape(SEQ, H, DR), places)
    key_content, values, key_turned, query_turned = lax.optimization_barrier((key_content, values, key_turned, query_turned))

    def subsets(inputs):
        shaped = inputs.reshape((N_SP, N_TP, per_device) + inputs.shape[1:])
        return jnp.swapaxes(shaped, 0, 1).reshape((N_TP, N_SP * per_device) + inputs.shape[1:])
    grouped = (subsets(key_content.reshape(SEQ, H, DN)), subsets(values.reshape(SEQ, H, DV)), subsets(key_turned), subsets(places))
    score_scale = 1.0 / math.sqrt(DN + DR)

    def one_block(query_block):
        contents, turned, query_places = query_block

        def one_subset(subset):
            key_rows, value_rows, key_turns, key_places = subset
            scores = (jnp.einsum('qhd,khd->qhk', contents.astype(jnp.float32), key_rows.astype(jnp.float32)) + jnp.einsum('qhr,kr->qhk', turned.astype(jnp.float32), key_turns.astype(jnp.float32))) * score_scale
            allowed = (key_places[None, :] // SPAN <= query_places[:, None] // SPAN)[:, None, :]
            highest = lax.optimization_barrier(jnp.max(jnp.where(allowed, scores, masked_score), axis=-1))
            weights = jnp.where(allowed, jnp.exp(scores - highest[..., None]), 0.0)
            weight_sum = lax.optimization_barrier(jnp.sum(weights, axis=-1))
            rounded = lax.optimization_barrier(weights.astype(jnp.bfloat16))
            weighted = jnp.einsum('qhk,khv->qhv', rounded.astype(jnp.float32), value_rows.astype(jnp.float32))
            return (highest, weight_sum, weighted)
        highest, weight_sum, weighted = lax.map(one_subset, grouped)
        overall = lax.optimization_barrier(jnp.max(highest, axis=0))
        factor = jnp.exp(highest - overall)
        merged = lax.optimization_barrier(jnp.sum(factor[..., None] * weighted, axis=0)) / lax.optimization_barrier(jnp.sum(factor * weight_sum, axis=0))[..., None]
        return merged.astype(jnp.bfloat16).reshape(TOK, H * DV)
    blocks = (query_content.reshape(N_SP, TOK, H, DN), query_turned.reshape(N_SP, TOK, H, DR), places.reshape(N_SP, TOK))
    head_out = lax.map(one_block, blocks).reshape(SEQ, H * DV)
    mixed_rows = (residual.astype(jnp.float32) + jnp.dot(head_out, out_proj, preferred_element_type=jnp.float32)).astype(jnp.bfloat16)
    mixed_rows = lax.optimization_barrier(mixed_rows)
    normed_rows = norm_round(mixed_rows, mixer_gain)
    hidden = (jax.nn.silu(jnp.dot(normed_rows, gate_proj, preferred_element_type=jnp.float32)) * jnp.dot(normed_rows, up_proj, preferred_element_type=jnp.float32)).astype(jnp.bfloat16)
    return (mixed_rows.astype(jnp.float32) + jnp.dot(hidden, down_proj, preferred_element_type=jnp.float32)).astype(jnp.bfloat16)
```

```python
import math

import jax
import jax.numpy as jnp
from jax import lax
from jax.sharding import Mesh, PartitionSpec as P

H = 8
DN = 128
DR = 64
DV = 128
SPAN = 64


epsilon = 1e-06
masked_score = -1e30
SP = ("g", "r")


def norm_round(inputs, scales):
    widened = inputs.astype(jnp.float32)
    factor = lax.rsqrt(jnp.mean(widened * widened, axis=-1, keepdims=True) + epsilon)
    return (widened * factor * scales).astype(jnp.bfloat16)


def rotate(inputs, places):
    dimension = inputs.shape[-1]
    middle = dimension // 2
    inverse = 10000.0 ** (-jnp.arange(0, dimension, 2, dtype=jnp.float32) / dimension)
    angles = places.astype(jnp.float32)[:, None, None] * inverse[None, None, :]
    cosine_table = jnp.cos(angles)
    sine_table = jnp.sin(angles)
    widened = inputs.astype(jnp.float32)
    first_half = widened[..., :middle]
    second_half = widened[..., middle:]
    return jnp.concatenate(
        [
            first_half * cosine_table - second_half * sine_table,
            second_half * cosine_table + first_half * sine_table,
        ],
        axis=-1,
    ).astype(jnp.bfloat16)


def shards(
    query_content,
    query_rotary,
    latents,
    key_rotary,
    latent_gain,
    key_up,
    value_up,
    out_proj,
    residual,
    mixer_gain,
    gate_proj,
    up_proj,
    down_proj,
):
    query_rows = query_content.shape[0]
    tp_count = lax.axis_size("tp")
    members = lax.axis_size("r")
    sp_index = lax.axis_index(SP)
    tp_index = lax.axis_index("tp")
    rank = latents.shape[1]
    heads = H // tp_count

    own_keys = jnp.concatenate([latents, key_rotary], axis=1)
    all_keys = lax.all_gather(own_keys, SP + ("tp",), axis=0, tiled=True)
    row_count = all_keys.shape[0]

    def pieces(weights):
        rows, columns = weights.shape
        shaped = weights.reshape(rows, members, columns // members)
        return jnp.swapaxes(shaped, 0, 1)

    gate_up = jnp.concatenate([pieces(gate_proj), pieces(up_proj)], axis=2)
    down = pieces(down_proj.T)
    gate_up = lax.all_to_all(gate_up, "r", split_axis=0, concat_axis=0, tiled=True)
    down = lax.all_to_all(down, "r", split_axis=0, concat_axis=0, tiled=True)
    gate_up = lax.all_gather(
        gate_up.reshape(-1, gate_up.shape[-1]), "g", axis=0, tiled=True
    )
    down = lax.all_gather(down.reshape(-1, down.shape[-1]), "g", axis=0, tiled=True)

    key_places = jnp.arange(row_count, dtype=jnp.int32)
    query_places = sp_index * query_rows + jnp.arange(query_rows, dtype=jnp.int32)
    normed = norm_round(all_keys[:, :rank], latent_gain)
    key_turned = rotate(all_keys[:, None, rank:], key_places)[:, 0, :]
    own_rotary = lax.dynamic_slice_in_dim(query_rotary, tp_index * heads * DR, heads * DR, 1)
    own_content = lax.dynamic_slice_in_dim(query_content, tp_index * heads * DN, heads * DN, 1)
    query_turned = rotate(own_rotary.reshape(query_rows, heads, DR), query_places)
    allowed = key_places[None, :] // SPAN <= query_places[:, None] // SPAN
    score_scale = 1.0 / math.sqrt(DN + DR)
    key_rows = jnp.dot(normed, key_up, preferred_element_type=jnp.float32).astype(jnp.bfloat16)
    value_rows = jnp.dot(normed, value_up, preferred_element_type=jnp.float32).astype(jnp.bfloat16)
    outs = []
    for h in range(heads):
        k = jnp.concatenate([key_rows[:, h * DN : (h + 1) * DN], key_turned], axis=1)
        q = jnp.concatenate(
            [own_content[:, h * DN : (h + 1) * DN], query_turned[:, h, :]], axis=1
        )
        scores = lax.dot_general(
            q, k, (((1,), (1,)), ((), ())), preferred_element_type=jnp.float32
        )
        scores = jnp.where(allowed, scores * score_scale, masked_score)
        highest = jnp.max(scores, axis=-1, keepdims=True)
        weights = jnp.where(allowed, jnp.exp(scores - highest), 0.0)
        weight_sum = jnp.sum(weights, axis=-1, keepdims=True)
        weighted = jnp.dot(
            weights.astype(jnp.bfloat16),
            value_rows[:, h * DV : (h + 1) * DV],
            preferred_element_type=jnp.float32,
        )
        outs.append((weighted / weight_sum).astype(jnp.bfloat16))
    own_heads = jnp.concatenate(outs, axis=1)
    attended = lax.all_gather(own_heads, "tp", axis=1, tiled=True)
    mixed_rows = (
        residual.astype(jnp.float32)
        + jnp.dot(attended, out_proj, preferred_element_type=jnp.float32)
    ).astype(jnp.bfloat16)
    whole_rows = lax.all_gather(mixed_rows, "tp", axis=1, tiled=True)
    normed_rows = norm_round(whole_rows, mixer_gain)
    group_rows = lax.all_gather(normed_rows, "r", axis=0, tiled=True)
    both = jnp.dot(group_rows, gate_up, preferred_element_type=jnp.float32)
    units = both.shape[1] // 2
    hidden = (jax.nn.silu(both[:, :units]) * both[:, units:]).astype(jnp.bfloat16)
    partial_value = lax.dot_general(
        hidden, down, (((1,), (1,)), ((), ())), preferred_element_type=jnp.float32
    ).astype(jnp.bfloat16)
    mixer_out = lax.psum_scatter(partial_value, "r", scatter_dimension=0, tiled=True)
    mixer_out = lax.psum_scatter(mixer_out, "tp", scatter_dimension=1, tiled=True)
    return (mixed_rows.astype(jnp.float32) + mixer_out.astype(jnp.float32)).astype(jnp.bfloat16)


def solution(mesh):
    sp_count, tp_count = mesh.shape["sp"], mesh.shape["tp"]
    members = math.gcd(sp_count, 4)
    grouped = Mesh(
        mesh.devices.reshape(sp_count // members, members, tp_count), SP + ("tp",)
    )
    return jax.shard_map(
        shards,
        mesh=grouped,
        in_specs=(
            P(SP, None),
            P(SP, None),
            P(SP + ("tp",), None),
            P(SP + ("tp",), None),
            P(),
            P(None, "tp"),
            P(None, "tp"),
            P(None, "tp"),
            P(SP, "tp"),
            P(),
            P(SP, "tp"),
            P(SP, "tp"),
            P("tp", SP),
        ),
        out_specs=P(SP, "tp"),
        check_vma=False,
    )
```

```python
import math

import jax
import jax.numpy as jnp
from jax import lax
from jax.sharding import Mesh, PartitionSpec as P

H = 8
DN = 128
DR = 64
DV = 128
SPAN = 64


epsilon = 1e-06
masked_score = -1e30
SP = ("z", "y", "c")


def norm_round(inputs, scales):
    widened = inputs.astype(jnp.float32)
    factor = lax.rsqrt(jnp.mean(widened * widened, axis=-1, keepdims=True) + epsilon)
    return (widened * factor * scales).astype(jnp.bfloat16)


def rotate(inputs, places):
    dimension = inputs.shape[-1]
    middle = dimension // 2
    inverse = 10000.0 ** (-jnp.arange(0, dimension, 2, dtype=jnp.float32) / dimension)
    angles = places.astype(jnp.float32)[:, None, None] * inverse[None, None, :]
    cosine_table = jnp.cos(angles)
    sine_table = jnp.sin(angles)
    widened = inputs.astype(jnp.float32)
    first_half = widened[..., :middle]
    second_half = widened[..., middle:]
    return jnp.concatenate(
        [
            first_half * cosine_table - second_half * sine_table,
            second_half * cosine_table + first_half * sine_table,
        ],
        axis=-1,
    ).astype(jnp.bfloat16)


def hop(inputs, axis, offset):
    count = lax.axis_size(axis)
    return lax.ppermute(inputs, axis, [(i, (i + offset) % count) for i in range(count)])


def others(inputs, axis):
    return [inputs] + [hop(inputs, axis, d) for d in range(1, lax.axis_size(axis))]


def take(inputs, index, count, dim):
    size = inputs.shape[dim] // count
    return lax.dynamic_slice_in_dim(inputs, index * size, size, dim)


def in_order(blocks, axis, dim):
    count, me = lax.axis_size(axis), lax.axis_index(axis)
    if count == 1:
        return blocks[0]
    if count == 2:
        straight = jnp.concatenate(blocks, axis=dim)
        turned = jnp.concatenate(blocks[::-1], axis=dim)
        return jnp.where(me == 0, straight, turned)
    size = blocks[0].shape[dim]
    shape = list(blocks[0].shape)
    shape[dim] = size * count
    result = jnp.zeros(shape, blocks[0].dtype)
    for d, block in enumerate(blocks):
        place = lax.rem(me - d + count, count) * size
        result = lax.dynamic_update_slice_in_dim(result, block, place, dim)
    return result


def shards(
    query_content,
    query_rotary,
    latents,
    key_rotary,
    latent_gain,
    key_up,
    value_up,
    out_proj,
    residual,
    mixer_gain,
    gate_proj,
    up_proj,
    down_proj,
):
    query_rows = query_content.shape[0]
    tp_count, z_count = lax.axis_size("tp"), lax.axis_size("z")
    sp_index, tp_index, z_index = (
        lax.axis_index(SP),
        lax.axis_index("tp"),
        lax.axis_index("z"),
    )
    rank = latents.shape[1]
    per_device = latents.shape[0]
    heads = H // tp_count

    gathered = jnp.concatenate([latents, key_rotary], axis=1)
    places = (sp_index * tp_count + tp_index) * per_device + jnp.arange(
        per_device, dtype=jnp.int32
    )
    strides = {
        "z": lax.axis_size("y") * lax.axis_size("c") * tp_count * per_device,
        "y": lax.axis_size("c") * tp_count * per_device,
        "c": tp_count * per_device,
        "tp": per_device,
    }
    pieces = []
    for weights in (gate_proj, up_proj, down_proj.T):
        rows, columns = weights.shape
        pieces.append(jnp.swapaxes(weights.reshape(rows, z_count, columns // z_count), 0, 1))
    for axis in ("z", "tp", "y", "c"):
        count, me = lax.axis_size(axis), lax.axis_index(axis)
        gathered = jnp.concatenate(others(gathered, axis), axis=0)
        places = jnp.concatenate(
            [places + (lax.rem(me - d + count, count) - me) * strides[axis] for d in range(count)]
        )
        if axis == "z":
            gathered, pieces = lax.optimization_barrier((gathered, pieces))

    whole = []
    for piece in pieces:
        rows, units = piece.shape[1:]
        blocks = []
        for d in range(z_count):
            block = take(piece, lax.rem(z_index + d, z_count), z_count, 0)
            blocks.append(hop(block, "z", d) if d else block)
        block = in_order(blocks, "z", 0)[:, None]
        block = in_order(others(block, "y"), "y", 1)[:, :, None]
        block = in_order(others(block, "c"), "c", 2)
        whole.append(block.reshape(-1, units))
    gate, up, down = whole

    query_places = sp_index * query_rows + jnp.arange(query_rows, dtype=jnp.int32)
    normed = norm_round(gathered[:, :rank], latent_gain)
    key_turned = rotate(gathered[:, None, rank:], places)[:, 0, :]
    own_rotary = take(query_rotary, tp_index, tp_count, 1)
    own_content = take(query_content, tp_index, tp_count, 1)
    query_turned = rotate(own_rotary.reshape(query_rows, heads, DR), query_places)
    allowed = places[None, :] // SPAN <= query_places[:, None] // SPAN
    score_scale = 1.0 / math.sqrt(DN + DR)
    key_rows = jnp.dot(normed, key_up, preferred_element_type=jnp.float32).astype(jnp.bfloat16)
    value_rows = jnp.dot(normed, value_up, preferred_element_type=jnp.float32).astype(jnp.bfloat16)
    outs = []
    for h in range(heads):
        k = jnp.concatenate([key_rows[:, h * DN : (h + 1) * DN], key_turned], axis=1)
        q = jnp.concatenate(
            [own_content[:, h * DN : (h + 1) * DN], query_turned[:, h, :]], axis=1
        )
        scores = lax.dot_general(
            q, k, (((1,), (1,)), ((), ())), preferred_element_type=jnp.float32
        )
        scores = jnp.where(allowed, scores * score_scale, masked_score)
        highest = jnp.max(scores, axis=-1, keepdims=True)
        weights = jnp.where(allowed, jnp.exp(scores - highest), 0.0)
        weight_sum = jnp.sum(weights, axis=-1, keepdims=True)
        weighted = jnp.dot(
            weights.astype(jnp.bfloat16),
            value_rows[:, h * DV : (h + 1) * DV],
            preferred_element_type=jnp.float32,
        )
        outs.append((weighted / weight_sum).astype(jnp.bfloat16))
    own_heads = jnp.concatenate(outs, axis=1)
    total = residual.astype(jnp.float32)
    for d, block in enumerate(others(own_heads, "tp")):
        part = take(out_proj, lax.rem(tp_index - d + tp_count, tp_count), tp_count, 0)
        total = total + jnp.dot(block, part, preferred_element_type=jnp.float32)
    mixed_rows = total.astype(jnp.bfloat16)

    result = mixed_rows.astype(jnp.float32)
    for d, rows in enumerate(others(mixed_rows, "z")):
        normed_rows = norm_round(in_order(others(rows, "tp"), "tp", 1), mixer_gain)
        hidden = (
            jax.nn.silu(jnp.dot(normed_rows, gate, preferred_element_type=jnp.float32))
            * jnp.dot(normed_rows, up, preferred_element_type=jnp.float32)
        ).astype(jnp.bfloat16)

        def share(index):
            part = take(down, lax.rem(index, tp_count), tp_count, 0)
            return lax.dot_general(
                hidden, part, (((1,), (1,)), ((), ())), preferred_element_type=jnp.float32
            )

        arrived = [
            hop(share(tp_index + e).astype(jnp.bfloat16), "tp", e) for e in range(1, tp_count)
        ]
        sums = share(tp_index)
        for part in arrived:
            sums = sums + part.astype(jnp.float32)
        if d:
            sums = hop(sums.astype(jnp.bfloat16), "z", -d).astype(jnp.float32)
        result = result + sums
    return result.astype(jnp.bfloat16)


def solution(mesh):
    sp_count, tp_count = mesh.shape["sp"], mesh.shape["tp"]
    grouped = Mesh(mesh.devices.reshape(sp_count // 4, 2, 2, tp_count), SP + ("tp",))
    return jax.shard_map(
        shards,
        mesh=grouped,
        in_specs=(
            P(SP, None),
            P(SP, None),
            P(SP + ("tp",), None),
            P(SP + ("tp",), None),
            P(),
            P(None, "tp"),
            P(None, "tp"),
            P(None, "tp"),
            P(SP, "tp"),
            P(),
            P(SP, "tp"),
            P(SP, "tp"),
            P("tp", SP),
        ),
        out_specs=P(SP, "tp"),
        check_vma=False,
    )
```
